32 devices in a mesh: sp: 8 (over z, y), tp: 4 (over x, core).
Axes of the slice: x: 2, y: 2, z: 4, core: 2. Of those that a mesh axis runs over, the one named last changes fastest.
Arguments:
- queries: bfloat16 [4096, 2048], P('sp', 'tp'), may hold values from -8 to 8
- keys: bfloat16 [4096, 512], P('sp', 'tp'), may hold values from -8 to 8
- values: bfloat16 [4096, 512], P('sp', 'tp'), may hold values from -6 to 6
- q_gain: float32 [128], replicated, may hold values from 0.1 to 5.8
- k_gain: float32 [128], replicated, may hold values from 0.1 to 5.8
- out_weight: bfloat16 [2048, 2048], replicated, may hold values from -0.125 to 0.125
- out_gain: float32 [2048], replicated, may hold values from 0.1 to 1.9
- residual_in: bfloat16 [4096, 2048], P(('sp', 'tp')), may hold values from -6 to 6
- mlp_gain: float32 [2048], replicated, may hold values from 0.1 to 1.9
- gate_weight: bfloat16 [2048, 5632], P('sp', 'tp'), may hold values from -0.125 to 0.125
- up_weight: bfloat16 [2048, 5632], P('sp', 'tp'), may hold values from -0.125 to 0.125
- down_weight: bfloat16 [5632, 2048], P('tp', 'sp'), may hold values from -0.078125 to 0.078125
- final_gain: float32 [2048], replicated, may hold values from 0.1 to 1.9
Outputs:
- layer_out: bfloat16 [4096, 2048], P(('sp', 'tp'))
The draws below stay inside these ranges and needn't reach their ends.
All inputs are finite; a program needn't handle non-finite values.
Results may differ from the reference program's by a relative error of at most 0.015.
The reference program's roundings to bfloat16 on the way count: a program that leaves them out, or rounds other values in their place, can miss the bound.
Values may be sent and summed in bfloat16 or wider, within the bound.
A program may use at most 128 MiB of HBM per device.

```python
import jax
import jax.numpy as jnp
from jax import lax

D = 2048
HQ = 16
KV = 4
HD = 128
FF = 5632
GRID_W = 64
TOK_DEV = 512
TOKENS = 4096


def drawn(base_key):
    query_base = jnp.clip(jax.random.normal(jax.random.fold_in(base_key, 101), (TOKENS, HQ, HD), jnp.float32), -6.0, 6.0)
    key_base = jnp.clip(jax.random.normal(jax.random.fold_in(base_key, 102), (TOKENS, KV, HD), jnp.float32), -6.0, 6.0)
    return (query_base.reshape(TOKENS, HQ * HD), key_base.reshape(TOKENS, KV * HD))


def gain_values(base_key):
    return 1.0 + 0.18 * jnp.clip(jax.random.normal(base_key, (HD,), jnp.float32), -5.0, 5.0)


def draw_queries(key, part):
    return drawn(key)[0].astype(jnp.bfloat16)


def draw_keys(key, part):
    return drawn(key)[1].astype(jnp.bfloat16)


def draw_q_gain(key, part):
    return gain_values(jax.random.fold_in(key, 201))


def draw_k_gain(key, part):
    return gain_values(jax.random.fold_in(key, 202))


def level_of(own_key, shape, shards, smallest, largest):
    gain, own = 1.0, jax.random.fold_in(own_key, 6)
    for position, shards_of in shards:
        draws = jnp.exp(jax.random.uniform(jax.random.fold_in(own, position), (shards_of,), jnp.float32, smallest / len(shards), largest / len(shards)))
        gain = gain * jnp.repeat(draws, shape[position] // shards_of).reshape([-1 if axis == position else 1 for axis in range(len(shape))])
    return gain


def scatter_about(key, extent, spread, bound, shards=(), kind=jnp.bfloat16):
    loudness = level_of(key, extent, shards, -0.22, 0.18) if shards else 1.0
    entries = jax.random.normal(key, extent, jnp.float32) * spread * loudness
    return jnp.minimum(jnp.maximum(entries, -bound), bound).astype(kind)


def setup_inputs(seed: int = 0) -> dict:
    splits = jax.random.split(jax.random.key(seed), 14)
    queries = draw_queries(jax.random.fold_in(splits[13], 71), 0)
    keys = draw_keys(jax.random.fold_in(splits[13], 71), 0)
    values = scatter_about(splits[2], (TOKENS, KV * HD), 1.0, 6.0, ((0, 8), (1, 4)))
    q_gain = draw_q_gain(jax.random.fold_in(splits[13], 71), 0)
    k_gain = draw_k_gain(jax.random.fold_in(splits[13], 71), 0)
    out_weight = scatter_about(splits[5], (HQ * HD, D), (HQ * HD) ** -0.5, 0.125)
    out_gain = jnp.clip(1.0 + 0.18 * jax.random.normal(splits[6], (D,), jnp.float32), 0.1, 1.9)
    residual_in = scatter_about(splits[7], (TOKENS, D), 1.0, 6.0, ((0, 32),))
    mlp_gain = jnp.clip(1.0 + 0.18 * jax.random.normal(splits[8], (D,), jnp.float32), 0.1, 1.9)
    gate_weight = scatter_about(splits[9], (D, FF), D ** -0.5, 0.125, ((0, 8), (1, 4)))
    up_weight = scatter_about(splits[10], (D, FF), D ** -0.5, 0.125, ((0, 8), (1, 4)))
    down_weight = scatter_about(splits[11], (FF, D), FF ** -0.5, 0.078125, ((0, 4), (1, 8)))
    final_gain = jnp.clip(1.0 + 0.18 * jax.random.normal(splits[12], (D,), jnp.float32), 0.1, 1.9)
    return dict(queries=queries, keys=keys, values=values, q_gain=q_gain, k_gain=k_gain, out_weight=out_weight, out_gain=out_gain, residual_in=residual_in, mlp_gain=mlp_gain, gate_weight=gate_weight, up_weight=up_weight, down_weight=down_weight, final_gain=final_gain)


def rms_scale(matrix):
    return matrix * lax.rsqrt(lax.optimization_barrier(jnp.mean(matrix * matrix, axis=-1, keepdims=True)) + 1e-06)

def rotary(matrix, positions):
    quarter = matrix.shape[-1] // 4
    freqs = 10000.0 ** (-jnp.arange(quarter, dtype=jnp.float32) / quarter)
    grid = jnp.stack([positions // GRID_W, positions % GRID_W], axis=-1).astype(jnp.float32)
    angle = grid[:, :, None] * freqs
    cosine = jnp.cos(angle)[:, None]
    sine = jnp.sin(angle)[:, None]
    parts = matrix.reshape(matrix.shape[:-1] + (2, 2, quarter))
    first = parts[..., 0, :]
    second = parts[..., 1, :]
    turned = jnp.stack([first * cosine - second * sine, second * cosine + first * sine], axis=-2)
    return turned.reshape(matrix.shape)

def reference(queries, keys, values, q_gain, k_gain, out_weight, out_gain, residual_in, mlp_gain, gate_weight, up_weight, down_weight, final_gain):
    tok_total = queries.shape[0]
    positions = jnp.arange(tok_total, dtype=jnp.int32)
    query_rot = rotary(rms_scale(queries.reshape(tok_total, HQ, HD).astype(jnp.float32)) * q_gain, positions).astype(jnp.bfloat16)
    key_rot = rotary(rms_scale(keys.reshape(tok_total, KV, HD).astype(jnp.float32)) * k_gain, positions).astype(jnp.bfloat16)
    value_heads = values.reshape(tok_total, KV, HD)
    group_size = HQ // KV
    score_scale = HD ** (-0.5)

    def one_head(head_index):
        query_head = lax.dynamic_index_in_dim(query_rot, head_index, 1, keepdims=False)
        key_head = lax.dynamic_index_in_dim(key_rot, head_index // group_size, 1, keepdims=False)
        value_head = lax.dynamic_index_in_dim(value_heads, head_index // group_size, 1, keepdims=False)

        def one_block(query_block):
            scores = jnp.dot(query_block, key_head.T, preferred_element_type=jnp.float32) * score_scale
            highest = lax.optimization_barrier(jnp.max(scores, axis=-1, keepdims=True))
            exp_scores = jnp.exp(scores - highest)
            weight_sum = lax.optimization_barrier(jnp.sum(exp_scores, axis=-1, keepdims=True))
            mixed = jnp.dot(exp_scores.astype(jnp.bfloat16), value_head, preferred_element_type=jnp.float32) / weight_sum
            return mixed.astype(jnp.bfloat16)
        blocks = query_head.reshape(tok_total // TOK_DEV, TOK_DEV, HD)
        return lax.map(one_block, blocks).reshape(tok_total, HD)
    per_head = lax.map(one_head, jnp.arange(HQ, dtype=jnp.int32))
    attended = jnp.transpose(per_head, (1, 0, 2)).reshape(tok_total, HQ * HD)
    projected = jnp.dot(attended, out_weight, preferred_element_type=jnp.float32)
    mid_stream = (residual_in.astype(jnp.float32) + out_gain * rms_scale(projected)).astype(jnp.bfloat16)
    normed = (mlp_gain * rms_scale(mid_stream.astype(jnp.float32))).astype(jnp.bfloat16)
    gate_proj = jnp.dot(normed, gate_weight, preferred_element_type=jnp.float32)
    up_proj = jnp.dot(normed, up_weight, preferred_element_type=jnp.float32)
    hidden = (jax.nn.silu(gate_proj) * up_proj).astype(jnp.bfloat16)
    mlp_branch = jnp.dot(hidden, down_weight, preferred_element_type=jnp.float32)
    return (mid_stream.astype(jnp.float32) + final_gain * rms_scale(mlp_branch)).astype(jnp.bfloat16)
```

```python
import functools
import math

import jax
import jax.numpy as jnp
from jax import lax
from jax.experimental import pallas as pl
from jax.experimental.pallas import tpu as pltpu
from jax.sharding import PartitionSpec as P

GRID_W = 64


def rms_scale(matrix):
    return matrix * lax.rsqrt(jnp.mean(matrix * matrix, axis=-1, keepdims=True) + 1e-06)


def rotary(matrix, positions):
    quarter = matrix.shape[-1] // 4
    freqs = 10000.0 ** (-jnp.arange(quarter, dtype=jnp.float32) / quarter)
    grid = jnp.stack([positions // GRID_W, positions % GRID_W], axis=-1).astype(jnp.float32)
    angle = grid[:, :, None] * freqs
    cosine = jnp.cos(angle)[:, None]
    sine = jnp.sin(angle)[:, None]
    parts = matrix.reshape(matrix.shape[:-1] + (2, 2, quarter))
    first = parts[..., 0, :]
    second = parts[..., 1, :]
    turned = jnp.stack([first * cosine - second * sine, second * cosine + first * sine], axis=-2)
    return turned.reshape(matrix.shape)


def on_device(
    queries,
    keys,
    values,
    q_gain,
    k_gain,
    out_weight,
    out_gain,
    residual_in,
    mlp_gain,
    gate_weight,
    up_weight,
    down_weight,
    final_gain,
):
    tok_rows = queries.shape[0]
    head_size = q_gain.shape[0]
    q_heads = queries.shape[1] // head_size
    kv_heads = keys.shape[1] // head_size
    group_size = q_heads // kv_heads
    positions = lax.axis_index("sp") * tok_rows + jnp.arange(tok_rows, dtype=jnp.int32)
    query_rot = rotary(
        rms_scale(queries.reshape(tok_rows, q_heads, head_size).astype(jnp.float32)) * q_gain,
        positions,
    ).astype(jnp.bfloat16)
    key_rot = rotary(
        rms_scale(keys.reshape(tok_rows, kv_heads, head_size).astype(jnp.float32)) * k_gain,
        positions,
    ).astype(jnp.bfloat16)
    key_flat = key_rot.reshape(tok_rows, kv_heads * head_size)
    grouped = query_rot.reshape(tok_rows, kv_heads, group_size, head_size)
    score_scale = head_size ** (-0.5)
    key_all, value_all = (
        lax.all_gather(key_flat, "sp", axis=0, tiled=True),
        lax.all_gather(values, "sp", axis=0, tiled=True),
    )
    total_rows = key_all.shape[0]
    span = math.gcd(total_rows, 1024)
    key_blocks = key_all.reshape(total_rows // span, span, kv_heads, head_size)
    value_blocks = value_all.reshape(total_rows // span, span, kv_heads, head_size)

    def step(run_state, blocks):
        highest, weight_sum, accum = run_state
        key_block, value_block = blocks
        scores = (
            jnp.einsum("qcgd,kcd->cgqk", grouped, key_block, preferred_element_type=jnp.float32)
            * score_scale
        )
        new_high = jnp.maximum(highest, jnp.max(scores, axis=-1))
        factor = jnp.exp(highest - new_high)
        exp_scores = jnp.exp(scores - new_high[..., None])
        weight_sum = weight_sum * factor + jnp.sum(exp_scores, axis=-1)
        accum = accum * factor[..., None] + jnp.einsum(
            "cgqk,kcd->cgqd",
            exp_scores.astype(jnp.bfloat16),
            value_block,
            preferred_element_type=jnp.float32,
        )
        return ((new_high, weight_sum, accum), None)

    start_state = (
        jnp.full((kv_heads, group_size, tok_rows), -1e30, jnp.float32),
        jnp.zeros((kv_heads, group_size, tok_rows), jnp.float32),
        jnp.zeros((kv_heads, group_size, tok_rows, head_size), jnp.float32),
    )
    final_state, unused = lax.scan(step, start_state, (key_blocks, value_blocks))
    highest, weight_sum, accum = final_state
    attended = (
        jnp.transpose(accum / weight_sum[..., None], (2, 0, 1, 3))
        .reshape(tok_rows, q_heads * head_size)
        .astype(jnp.bfloat16)
    )
    head_rows = lax.all_to_all(attended, "tp", split_axis=0, concat_axis=1, tiled=True)
    projected = jnp.dot(head_rows, out_weight, preferred_element_type=jnp.float32)
    mid_stream = (residual_in.astype(jnp.float32) + out_gain * rms_scale(projected)).astype(
        jnp.bfloat16
    )
    normed = (mlp_gain * rms_scale(mid_stream.astype(jnp.float32))).astype(jnp.bfloat16)
    mixer_in = lax.all_gather(normed, "tp", axis=0, tiled=True)
    gate_proj = jnp.dot(
        mixer_in,
        lax.all_gather(gate_weight, "sp", axis=0, tiled=True),
        preferred_element_type=jnp.float32,
    )
    up_proj = jnp.dot(
        mixer_in,
        lax.all_gather(up_weight, "sp", axis=0, tiled=True),
        preferred_element_type=jnp.float32,
    )
    down_full = lax.all_gather(down_weight, "sp", axis=1, tiled=True)
    hidden = (jax.nn.silu(gate_proj) * up_proj).astype(jnp.bfloat16)
    mlp_branch = lax.psum_scatter(
        jnp.dot(hidden, down_full, preferred_element_type=jnp.float32).astype(jnp.bfloat16),
        "tp",
        scatter_dimension=0,
        tiled=True,
    ).astype(jnp.float32)
    return (mid_stream.astype(jnp.float32) + final_gain * rms_scale(mlp_branch)).astype(
        jnp.bfloat16
    )


MESH = pl.DeviceIdType.MESH
EPS = 1e-06


def layer_kernel(
    n,
    tn,
    q_in,
    k_in,
    v_hbm,
    cos_ref,
    sin_ref,
    qg_ref,
    kg_ref,
    ow_hbm,
    og_ref,
    res_ref,
    mg_ref,
    gate_hbm,
    up_hbm,
    down_hbm,
    fg_ref,
    out_ref,
    qs,
    kbuf,
    vbuf,
    gbuf,
    ubuf,
    dbuf,
    ow,
    m_s,
    l_s,
    acc,
    att,
    heads,
    proj,
    mid,
    mix,
    gacc,
    uacc,
    hid,
    pbuf,
    rbuf,
    loc_sem,
    send_sem,
    recv_sem,
    tp_send,
    tp_recv,
    pt_send,
    pt_recv,
):
    sp = lax.axis_index("sp")
    tp = lax.axis_index("tp")
    half = n // 2

    def ring_at(pos):
        pos = lax.rem(pos + 2 * n, n)
        return jnp.where(pos < half, 2 * pos, 2 * (n - 1 - pos) + 1)

    pos = jnp.where(lax.rem(sp, 2) == 0, sp // 2, n - 1 - sp // 2)
    right, left = ring_at(pos + 1), ring_at(pos - 1)
    tok, hd = k_in.shape
    groups = q_in.shape[1] // hd
    depth = gate_hbm.shape[0]
    hidden = gate_hbm.shape[1]
    rows = res_ref.shape[0]
    width = groups * hd

    locs = {
        "v": pltpu.make_async_copy(v_hbm, vbuf.at[sp], loc_sem.at[0]),
        "g": pltpu.make_async_copy(gate_hbm, gbuf.at[sp], loc_sem.at[1]),
        "u": pltpu.make_async_copy(up_hbm, ubuf.at[sp], loc_sem.at[2]),
        "d": pltpu.make_async_copy(down_hbm, dbuf.at[sp], loc_sem.at[3]),
        "o": pltpu.make_async_copy(ow_hbm, ow, loc_sem.at[4]),
    }
    for name in "vgudo":
        locs[name].start()

    lane = lax.broadcasted_iota(jnp.int32, (tok, hd), 1)
    quarter = hd // 4
    first = lax.rem(lane, 2 * quarter) < quarter

    def turned(x, gain):
        x = x.astype(jnp.float32)
        x = x * lax.rsqrt(jnp.mean(x * x, axis=-1, keepdims=True) + EPS) * gain
        other = jnp.where(first, pltpu.roll(x, hd - quarter, 1), pltpu.roll(x, quarter, 1))
        return (x * cos_ref[...] + other * sin_ref[...]).astype(jnp.bfloat16)

    kbuf[sp] = turned(k_in[...], kg_ref[...])

    barrier = pltpu.get_barrier_semaphore()
    for peer in (left, right):
        pl.semaphore_signal(barrier, inc=1, device_id=(peer, tp), device_id_type=MESH)
    for d in range(1, tn):
        pl.semaphore_signal(
            barrier, inc=1, device_id=(sp, lax.rem(tp + d, tn)), device_id_type=MESH
        )
    pl.semaphore_wait(barrier, 2 + tn - 1)

    cut = hidden // 2
    items = {
        "k": (0, half, lambda s: kbuf.at[s]),
        "v": (1, half - 1, lambda s: vbuf.at[s]),
        "g": (2, half, lambda s: gbuf.at[s]),
        "u": (3, half - 1, lambda s: ubuf.at[s]),
        "a": (4, half, lambda s: dbuf.at[s, pl.ds(0, cut), :]),
        "b": (5, half - 1, lambda s: dbuf.at[s, pl.ds(cut, hidden - cut), :]),
    }
    started = []

    def copies(name, step):
        number, to_right, view = items[name]
        found = []
        for way, count in ((0, to_right), (1, n - 1 - to_right)):
            if step > count:
                continue
            origin = ring_at(pos - (step - 1)) if way == 0 else ring_at(pos + (step - 1))
            index = (number * 2 + way) * half + step - 1
            found.append(
                pltpu.make_async_remote_copy(
                    src_ref=view(origin),
                    dst_ref=view(origin),
                    send_sem=send_sem.at[index],
                    recv_sem=recv_sem.at[index],
                    device_id=(right if way == 0 else left, tp),
                    device_id_type=MESH,
                )
            )
        return found

    def send(name, step):
        for copy in copies(name, step):
            copy.start()
            started.append(copy)

    def arrive(name, step, then=True):
        number, to_right, view = items[name]
        for way, count in ((0, to_right), (1, n - 1 - to_right)):
            if step > count:
                continue
            origin = ring_at(pos - step) if way == 0 else ring_at(pos + step)
            index = (number * 2 + way) * half + step - 1
            pltpu.make_async_remote_copy(
                src_ref=view(origin),
                dst_ref=view(origin),
                send_sem=send_sem.at[index],
                recv_sem=recv_sem.at[index],
                device_id=(right if way == 0 else left, tp),
                device_id_type=MESH,
            ).wait_recv()
            if step < count:
                index += 1
                copy = pltpu.make_async_remote_copy(
                    src_ref=view(origin),
                    dst_ref=view(origin),
                    send_sem=send_sem.at[index],
                    recv_sem=recv_sem.at[index],
                    device_id=(right if way == 0 else left, tp),
                    device_id_type=MESH,
                )
                copy.start()
                started.append(copy)

    send("k", 1)
    locs["v"].wait()
    send("v", 1)
    locs["g"].wait()
    send("g", 1)

    for h in range(groups):
        qs[h] = turned(q_in[:, h * hd : (h + 1) * hd], qg_ref[...])
    m_s[...] = jnp.full_like(m_s, -1e30)
    l_s[...] = jnp.zeros_like(l_s)
    acc[...] = jnp.zeros_like(acc)
    factor = hd ** (-0.5) * math.log2(math.e)

    def attend(slots):
        def one(i, carry):
            h = lax.rem(i, groups)
            slot = slots[0]
            if len(slots) > 1:
                slot = jnp.where(i < groups, slots[0], slots[1])
            scores = lax.dot_general(
                qs[h], kbuf[slot], (((1,), (1,)), ((), ())), preferred_element_type=jnp.float32
            )
            before = m_s[h]
            highest = jnp.maximum(before, jnp.max(scores, axis=-1, keepdims=True))
            scale = jnp.exp2((before - highest) * factor)
            probs = jnp.exp2((scores - highest) * factor)
            m_s[h] = highest
            l_s[h] = l_s[h] * scale + jnp.sum(probs, axis=-1, keepdims=True)
            acc[h] = acc[h] * scale + jnp.dot(
                probs.astype(jnp.bfloat16), vbuf[slot], preferred_element_type=jnp.float32
            )
            return carry

        lax.fori_loop(0, groups * len(slots), one, 0)

    attend([sp])
    for step in range(1, half + 1):
        arrive("k", step)
        arrive("v", step)
        if step == 1:
            locs["u"].wait()
            send("u", 1)
            locs["d"].wait()
        elif step >= 2:
            arrive("gu"[step % 2], step // 2 if step % 2 == 0 else (step - 1) // 2)
        ends = [ring_at(pos - step), ring_at(pos + step)]
        attend(ends if step < half else ends[:1])

    for h in range(groups):
        done = (acc[h] / l_s[h]).astype(jnp.bfloat16)
        for t in range(tn):
            att[t, :, h * hd : (h + 1) * hd] = done[t * rows : (t + 1) * rows]
    to_heads = []
    for d in range(1, tn):
        peer = lax.rem(tp + d, tn)
        copy = pltpu.make_async_remote_copy(
            src_ref=att.at[peer],
            dst_ref=heads.at[tp],
            send_sem=tp_send.at[d - 1],
            recv_sem=tp_recv.at[d - 1],
            device_id=(sp, peer),
            device_id_type=MESH,
        )
        copy.start()
        to_heads.append(copy)
    heads[tp] = att[tp]
    late = [(name, step) for step in range(1, half + 1) for name in "gu"]
    seen = [("gu"[s % 2], s // 2 if s % 2 == 0 else (s - 1) // 2) for s in range(2, half + 1)]
    late = [event for event in late if event not in seen]
    locs["o"].wait()
    for copy in to_heads:
        copy.wait_recv()

    span = math.gcd(ow.shape[1], 512)

    def project(i, carry):
        cols = pl.ds(pl.multiple_of(i * span, span), span)
        total = jnp.zeros((rows, span), jnp.float32)
        for t in range(tn):
            total += jnp.dot(
                heads[t], ow[t * width : (t + 1) * width, cols], preferred_element_type=jnp.float32
            )
        proj[:, cols] = total
        return carry

    lax.fori_loop(0, ow.shape[1] // span, project, 0)
    projected = proj[...]
    middle = (
        res_ref[...].astype(jnp.float32)
        + og_ref[...]
        * (projected * lax.rsqrt(jnp.mean(projected * projected, axis=-1, keepdims=True) + EPS))
    ).astype(jnp.bfloat16)
    mid[...] = middle
    middle = middle.astype(jnp.float32)
    normed = (
        mg_ref[...] * (middle * lax.rsqrt(jnp.mean(middle * middle, axis=-1, keepdims=True) + EPS))
    ).astype(jnp.bfloat16)
    mine = pl.ds(pl.multiple_of(tp * rows, rows), rows)
    for s in range(n):
        mix[s, mine, :] = normed[:, s * depth : (s + 1) * depth]
    to_mix = []
    for d in range(1, tn):
        peer = lax.rem(tp + d, tn)
        copy = pltpu.make_async_remote_copy(
            src_ref=mix.at[:, mine, :],
            dst_ref=mix.at[:, mine, :],
            send_sem=tp_send.at[tn - 1 + d - 1],
            recv_sem=tp_recv.at[tn - 1 + d - 1],
            device_id=(sp, peer),
            device_id_type=MESH,
        )
        copy.start()
        to_mix.append(copy)

    for event in late[: len(late) // 2]:
        arrive(*event)
    send("a", 1)
    send("b", 1)
    gacc[...] = jnp.zeros_like(gacc)
    uacc[...] = jnp.zeros_like(uacc)
    for copy in to_mix:
        copy.wait_recv()
    tile = math.gcd(tok, 256)

    def add_block(buf, total, slot):
        def one(i, carry):
            part = pl.ds(pl.multiple_of(i * tile, tile), tile)
            total[part, :] += jnp.dot(
                mix[slot, part, :], buf[slot], preferred_element_type=jnp.float32
            )
            return carry

        lax.fori_loop(0, tok // tile, one, 0)

    def add_blocks(name, slots):
        buf, total = (gbuf, gacc) if name == "g" else (ubuf, uacc)
        slots = list(slots)

        def one(i, carry):
            slot = slots[0]
            for place, other in enumerate(slots[1:]):
                slot = jnp.where(i > place, other, slot)
            add_block(buf, total, slot)
            return carry

        lax.fori_loop(0, len(slots), one, 0)

    def origins(name, step):
        to_right = items[name][1]
        found = []
        if step <= to_right:
            found.append(ring_at(pos - step))
        if step <= n - 1 - to_right:
            found.append(ring_at(pos + step))
        return found

    ready = {"g": [sp], "u": [sp]}
    for name, step in seen + late[: len(late) // 2]:
        ready[name] += origins(name, step)
    for name in "gu":
        add_blocks(name, ready[name])
    for name, step in late[len(late) // 2 :]:
        arrive(name, step)
        add_blocks(name, origins(name, step))

    def activate(i, carry):
        part = pl.ds(pl.multiple_of(i * 64, 64), 64)
        gate = gacc[part, :]
        hid[part, :] = (gate / (1.0 + jnp.exp(-gate)) * uacc[part, :]).astype(jnp.bfloat16)
        return carry

    lax.fori_loop(0, tok // 64, activate, 0)

    def shares(number, slot):
        def one(t, carry):
            part = pl.ds(pl.multiple_of(t * rows, rows), rows)
            pbuf[slot, t] = jnp.dot(
                hid[part, :], dbuf[slot], preferred_element_type=jnp.float32
            ).astype(jnp.bfloat16)
            return carry

        lax.fori_loop(0, tn, one, 0)
        for d in range(1, tn):
            peer = lax.rem(tp + d, tn)
            index = number * (tn - 1) + d - 1
            copy = pltpu.make_async_remote_copy(
                src_ref=pbuf.at[slot, peer],
                dst_ref=rbuf.at[tp, slot],
                send_sem=pt_send.at[index],
                recv_sem=pt_recv.at[index],
                device_id=(sp, peer),
                device_id_type=MESH,
            )
            copy.start()
            last.append(copy)
        rbuf[tp, slot] = pbuf[slot, tp]

    last = []
    shares(0, sp)
    number = 1
    for step in range(1, half + 1):
        arrive("a", step)
        arrive("b", step)
        if step < half:
            for slot in (ring_at(pos - step), ring_at(pos + step)):
                shares(number, slot)
                number += 1
        else:
            shares(number, ring_at(pos - step))
    for copy in last:
        copy.wait_recv()
    square = jnp.zeros((rows, 1), jnp.float32)
    for s in range(n):
        total = rbuf[0, s].astype(jnp.float32)
        for t in range(1, tn):
            total += rbuf[t, s].astype(jnp.float32)
        proj[:, s * depth : (s + 1) * depth] = total
        square += jnp.sum(total * total, axis=-1, keepdims=True)
    scale = lax.rsqrt(square / (n * depth) + EPS)
    out_ref[...] = (mid[...].astype(jnp.float32) + fg_ref[...] * (proj[...] * scale)).astype(
        jnp.bfloat16
    )
    for copy in started + to_heads + to_mix + last:
        copy.wait_send()


def rotary_tables(tok_rows, head_size):
    quarter = head_size // 4
    positions = lax.axis_index("sp") * tok_rows + jnp.arange(tok_rows, dtype=jnp.int32)
    lane = jnp.arange(head_size, dtype=jnp.int32)
    freqs = 10000.0 ** (-(lane % quarter).astype(jnp.float32) / quarter)
    row = (positions // GRID_W).astype(jnp.float32)[:, None]
    column = (positions % GRID_W).astype(jnp.float32)[:, None]
    angle = jnp.where(lane < 2 * quarter, row, column) * freqs
    sine = jnp.sin(angle)
    return jnp.cos(angle), jnp.where(lane % (2 * quarter) < quarter, -sine, sine)


def fused(n, tn, *args):
    (queries, keys, values, q_gain, k_gain, out_weight, out_gain, residual_in) = args[:8]
    (mlp_gain, gate_weight, up_weight, down_weight, final_gain) = args[8:]
    tok, hd = keys.shape
    groups = queries.shape[1] // hd
    depth, hidden = gate_weight.shape
    rows, wide = residual_in.shape
    cosine, sine = rotary_tables(tok, hd)
    vmem = pl.BlockSpec(memory_space=pltpu.VMEM)
    hbm = pl.BlockSpec(memory_space=pl.ANY)
    half = n // 2
    b16, f32 = jnp.bfloat16, jnp.float32
    return pl.pallas_call(
        functools.partial(layer_kernel, n, tn),
        out_shape=jax.ShapeDtypeStruct((rows, wide), b16),
        in_specs=[vmem, vmem, hbm, vmem, vmem, vmem, vmem, hbm, vmem, vmem, vmem, hbm, hbm, hbm, vmem],
        out_specs=vmem,
        scratch_shapes=[
            pltpu.VMEM((groups, tok, hd), b16),
            pltpu.VMEM((n, tok, hd), b16),
            pltpu.VMEM((n, tok, hd), b16),
            pltpu.VMEM((n, depth, hidden), b16),
            pltpu.VMEM((n, depth, hidden), b16),
            pltpu.VMEM((n, hidden, depth), b16),
            pltpu.VMEM((wide, wide), b16),
            pltpu.VMEM((groups, tok, 1), f32),
            pltpu.VMEM((groups, tok, 1), f32),
            pltpu.VMEM((groups, tok, hd), f32),
            pltpu.VMEM((tn, rows, groups * hd), b16),
            pltpu.VMEM((tn, rows, groups * hd), b16),
            pltpu.VMEM((rows, wide), f32),
            pltpu.VMEM((rows, wide), b16),
            pltpu.VMEM((n, tok, depth), b16),
            pltpu.VMEM((tok, hidden), f32),
            pltpu.VMEM((tok, hidden), f32),
            pltpu.VMEM((tok, hidden), b16),
            pltpu.VMEM((n, tn, rows, depth), b16),
            pltpu.VMEM((tn, n, rows, depth), b16),
            pltpu.SemaphoreType.DMA((5,)),
            pltpu.SemaphoreType.DMA((12 * half,)),
            pltpu.SemaphoreType.DMA((12 * half,)),
            pltpu.SemaphoreType.DMA((2 * (tn - 1),)),
            pltpu.SemaphoreType.DMA((2 * (tn - 1),)),
            pltpu.SemaphoreType.DMA((n * (tn - 1),)),
            pltpu.SemaphoreType.DMA((n * (tn - 1),)),
        ],
        compiler_params=pltpu.CompilerParams(
            collective_id=0, has_side_effects=True, vmem_limit_bytes=67043328
        ),
    )(
        queries,
        keys,
        values,
        cosine,
        sine,
        q_gain[None],
        k_gain[None],
        out_weight,
        out_gain[None],
        residual_in,
        mlp_gain[None],
        gate_weight,
        up_weight,
        down_weight,
        final_gain[None],
    )


def body(mesh, *args):
    n, tn = mesh.shape["sp"], mesh.shape["tp"]
    tok, hd = args[1].shape
    depth, hidden = args[9].shape
    fits = n % 2 == 0 and 4 <= n <= 8 and depth % 128 == 0 and hidden % 32 == 0
    if fits and tok % 256 == 0 and hd == 128:
        return fused(n, tn, *args)
    return on_device(*args)


def solution(mesh):
    return jax.shard_map(
        functools.partial(body, mesh),
        mesh=mesh,
        in_specs=(
            P("sp", "tp"),
            P("sp", "tp"),
            P("sp", "tp"),
            P(),
            P(),
            P(),
            P(),
            P(("sp", "tp"), None),
            P(),
            P("sp", "tp"),
            P("sp", "tp"),
            P("tp", "sp"),
            P(),
        ),
        out_specs=P(("sp", "tp"), None),
        check_vma=False,
    )
```

```python
import functools
import math

import jax
import jax.numpy as jnp
from jax import lax
from jax.experimental import pallas as pl
from jax.experimental.pallas import tpu as pltpu
from jax.sharding import PartitionSpec as P

GRID_W = 64


def rms_scale(matrix):
    return matrix * lax.rsqrt(jnp.mean(matrix * matrix, axis=-1, keepdims=True) + 1e-06)


def rotary(matrix, positions):
    quarter = matrix.shape[-1] // 4
    freqs = 10000.0 ** (-jnp.arange(quarter, dtype=jnp.float32) / quarter)
    grid = jnp.stack([positions // GRID_W, positions % GRID_W], axis=-1).astype(jnp.float32)
    angle = grid[:, :, None] * freqs
    cosine = jnp.cos(angle)[:, None]
    sine = jnp.sin(angle)[:, None]
    parts = matrix.reshape(matrix.shape[:-1] + (2, 2, quarter))
    first = parts[..., 0, :]
    second = parts[..., 1, :]
    turned = jnp.stack([first * cosine - second * sine, second * cosine + first * sine], axis=-2)
    return turned.reshape(matrix.shape)


def on_device(
    queries,
    keys,
    values,
    q_gain,
    k_gain,
    out_weight,
    out_gain,
    residual_in,
    mlp_gain,
    gate_weight,
    up_weight,
    down_weight,
    final_gain,
):
    tok_rows = queries.shape[0]
    head_size = q_gain.shape[0]
    q_heads = queries.shape[1] // head_size
    kv_heads = keys.shape[1] // head_size
    group_size = q_heads // kv_heads
    positions = lax.axis_index("sp") * tok_rows + jnp.arange(tok_rows, dtype=jnp.int32)
    query_rot = rotary(
        rms_scale(queries.reshape(tok_rows, q_heads, head_size).astype(jnp.float32)) * q_gain,
        positions,
    ).astype(jnp.bfloat16)
    key_rot = rotary(
        rms_scale(keys.reshape(tok_rows, kv_heads, head_size).astype(jnp.float32)) * k_gain,
        positions,
    ).astype(jnp.bfloat16)
    key_flat = key_rot.reshape(tok_rows, kv_heads * head_size)
    grouped = query_rot.reshape(tok_rows, kv_heads, group_size, head_size)
    score_scale = head_size ** (-0.5)
    key_all, value_all = (
        lax.all_gather(key_flat, "sp", axis=0, tiled=True),
        lax.all_gather(values, "sp", axis=0, tiled=True),
    )
    total_rows = key_all.shape[0]
    span = math.gcd(total_rows, 1024)
    key_blocks = key_all.reshape(total_rows // span, span, kv_heads, head_size)
    value_blocks = value_all.reshape(total_rows // span, span, kv_heads, head_size)

    def step(run_state, blocks):
        highest, weight_sum, accum = run_state
        key_block, value_block = blocks
        scores = (
            jnp.einsum("qcgd,kcd->cgqk", grouped, key_block, preferred_element_type=jnp.float32)
            * score_scale
        )
        new_high = jnp.maximum(highest, jnp.max(scores, axis=-1))
        factor = jnp.exp(highest - new_high)
        exp_scores = jnp.exp(scores - new_high[..., None])
        weight_sum = weight_sum * factor + jnp.sum(exp_scores, axis=-1)
        accum = accum * factor[..., None] + jnp.einsum(
            "cgqk,kcd->cgqd",
            exp_scores.astype(jnp.bfloat16),
            value_block,
            preferred_element_type=jnp.float32,
        )
        return ((new_high, weight_sum, accum), None)

    start_state = (
        jnp.full((kv_heads, group_size, tok_rows), -1e30, jnp.float32),
        jnp.zeros((kv_heads, group_size, tok_rows), jnp.float32),
        jnp.zeros((kv_heads, group_size, tok_rows, head_size), jnp.float32),
    )
    final_state, unused = lax.scan(step, start_state, (key_blocks, value_blocks))
    highest, weight_sum, accum = final_state
    attended = (
        jnp.transpose(accum / weight_sum[..., None], (2, 0, 1, 3))
        .reshape(tok_rows, q_heads * head_size)
        .astype(jnp.bfloat16)
    )
    head_rows = lax.all_to_all(attended, "tp", split_axis=0, concat_axis=1, tiled=True)
    projected = jnp.dot(head_rows, out_weight, preferred_element_type=jnp.float32)
    mid_stream = (residual_in.astype(jnp.float32) + out_gain * rms_scale(projected)).astype(
        jnp.bfloat16
    )
    normed = (mlp_gain * rms_scale(mid_stream.astype(jnp.float32))).astype(jnp.bfloat16)
    mixer_in = lax.all_gather(normed, "tp", axis=0, tiled=True)
    gate_proj = jnp.dot(
        mixer_in,
        lax.all_gather(gate_weight, "sp", axis=0, tiled=True),
        preferred_element_type=jnp.float32,
    )
    up_proj = jnp.dot(
        mixer_in,
        lax.all_gather(up_weight, "sp", axis=0, tiled=True),
        preferred_element_type=jnp.float32,
    )
    down_full = lax.all_gather(down_weight, "sp", axis=1, tiled=True)
    hidden = (jax.nn.silu(gate_proj) * up_proj).astype(jnp.bfloat16)
    mlp_branch = lax.psum_scatter(
        jnp.dot(hidden, down_full, preferred_element_type=jnp.float32).astype(jnp.bfloat16),
        "tp",
        scatter_dimension=0,
        tiled=True,
    ).astype(jnp.float32)
    return (mid_stream.astype(jnp.float32) + final_gain * rms_scale(mlp_branch)).astype(
        jnp.bfloat16
    )


MESH = pl.DeviceIdType.MESH
EPS = 1e-06


def layer_kernel(
    n,
    tn,
    q_in,
    k_in,
    v_hbm,
    cos_ref,
    sin_ref,
    qg_ref,
    kg_ref,
    ow_hbm,
    og_ref,
    res_ref,
    mg_ref,
    gate_hbm,
    up_hbm,
    down_hbm,
    fg_ref,
    out_ref,
    qs,
    kbuf,
    vbuf,
    raw,
    wt,
    wall,
    ow,
    m_s,
    l_s,
    acc,
    att,
    heads,
    proj,
    mid,
    toks,
    osc,
    psend,
    precv,
    loc_sem,
    send_sem,
    recv_sem,
    tp_send,
    tp_recv,
    a_send,
    a_recv,
    w_send,
    w_recv,
    t_send,
    t_recv,
    p_send,
    p_recv,
):
    sp = lax.axis_index("sp")
    tp = lax.axis_index("tp")
    half = n // 2

    def ring_at(pos):
        pos = lax.rem(pos + 2 * n, n)
        return jnp.where(pos < half, 2 * pos, 2 * (n - 1 - pos) + 1)

    pos = jnp.where(lax.rem(sp, 2) == 0, sp // 2, n - 1 - sp // 2)
    right, left = ring_at(pos + 1), ring_at(pos - 1)
    tok, hd = k_in.shape
    groups = q_in.shape[1] // hd
    depth = gate_hbm.shape[0]
    hidden = gate_hbm.shape[1]
    rows = res_ref.shape[0]
    width = groups * hd
    chunk = hidden // n
    side = rows // 2

    locs = {
        "v": pltpu.make_async_copy(v_hbm, vbuf.at[sp], loc_sem.at[0]),
        "g": pltpu.make_async_copy(gate_hbm, raw.at[0], loc_sem.at[1]),
        "u": pltpu.make_async_copy(up_hbm, raw.at[1], loc_sem.at[2]),
        "d": pltpu.make_async_copy(down_hbm, wt.at[2], loc_sem.at[3]),
        "o": pltpu.make_async_copy(ow_hbm, ow, loc_sem.at[4]),
    }
    for name in "vgudo":
        locs[name].start()

    lane = lax.broadcasted_iota(jnp.int32, (tok, hd), 1)
    quarter = hd // 4
    first = lax.rem(lane, 2 * quarter) < quarter

    def turned(x, gain):
        x = x.astype(jnp.float32)
        x = x * lax.rsqrt(jnp.mean(x * x, axis=-1, keepdims=True) + EPS) * gain
        other = jnp.where(first, pltpu.roll(x, hd - quarter, 1), pltpu.roll(x, quarter, 1))
        return (x * cos_ref[...] + other * sin_ref[...]).astype(jnp.bfloat16)

    kbuf[sp] = turned(k_in[...], kg_ref[...])

    barrier = pltpu.get_barrier_semaphore()
    for d in range(1, n):
        pl.semaphore_signal(
            barrier, inc=1, device_id=(lax.rem(sp + d, n), tp), device_id_type=MESH
        )
    for d in range(1, tn):
        pl.semaphore_signal(
            barrier, inc=1, device_id=(sp, lax.rem(tp + d, tn)), device_id_type=MESH
        )
    pl.semaphore_wait(barrier, n - 1 + tn - 1)

    items = {
        "k": (0, half, lambda s: kbuf.at[s]),
        "v": (1, half - 1, lambda s: vbuf.at[s]),
    }
    started = []

    def copies(name, step):
        number, to_right, view = items[name]
        found = []
        for way, count in ((0, to_right), (1, n - 1 - to_right)):
            if step > count:
                continue
            origin = ring_at(pos - (step - 1)) if way == 0 else ring_at(pos + (step - 1))
            index = (number * 2 + way) * half + step - 1
            found.append(
                pltpu.make_async_remote_copy(
                    src_ref=view(origin),
                    dst_ref=view(origin),
                    send_sem=send_sem.at[index],
                    recv_sem=recv_sem.at[index],
                    device_id=(right if way == 0 else left, tp),
                    device_id_type=MESH,
                )
            )
        return found

    def send(name, step):
        for copy in copies(name, step):
            copy.start()
            started.append(copy)

    def arrive(name, step, then=True):
        number, to_right, view = items[name]
        for way, count in ((0, to_right), (1, n - 1 - to_right)):
            if step > count:
                continue
            origin = ring_at(pos - step) if way == 0 else ring_at(pos + step)
            index = (number * 2 + way) * half + step - 1
            pltpu.make_async_remote_copy(
                src_ref=view(origin),
                dst_ref=view(origin),
                send_sem=send_sem.at[index],
                recv_sem=recv_sem.at[index],
                device_id=(right if way == 0 else left, tp),
                device_id_type=MESH,
            ).wait_recv()
            if step < count:
                index += 1
                copy = pltpu.make_async_remote_copy(
                    src_ref=view(origin),
                    dst_ref=view(origin),
                    send_sem=send_sem.at[index],
                    recv_sem=recv_sem.at[index],
                    device_id=(right if way == 0 else left, tp),
                    device_id_type=MESH,
                )
                copy.start()
                started.append(copy)

    send("k", 1)
    locs["v"].wait()
    send("v", 1)
    locs["g"].wait()
    locs["u"].wait()

    def transpose(i, carry):
        part = pl.ds(pl.multiple_of(i * 128, 128), 128)
        for which in range(2):
            wt[which, part, :] = raw[which, :, part].T
        return carry

    lax.fori_loop(0, hidden // 128, transpose, 0)
    locs["d"].wait()

    def units(index):
        return pl.ds(pl.multiple_of(index * chunk, 16), chunk)

    own_piece = pltpu.make_async_copy(
        wt.at[:, units(sp), :], wall.at[sp, :, units(tp), :], loc_sem.at[5]
    )
    own_piece.start()

    def spread(d):
        peer = lax.rem(sp + d, n)
        copy = pltpu.make_async_remote_copy(
            src_ref=wt.at[:, units(peer), :],
            dst_ref=wall.at[sp, :, units(tp), :],
            send_sem=a_send.at[d - 1],
            recv_sem=a_recv.at[d - 1],
            device_id=(peer, tp),
            device_id_type=MESH,
        )
        copy.start()
        started.append(copy)

    across, beside = lax.rem(tp + tn // 2, tn), tp + 1 - 2 * lax.rem(tp, 2)

    def relay(kind, d):
        slot = lax.rem(sp - d + n, n)
        owner = across if kind == 2 else tp
        piece = wall.at[slot, :, units(owner), :]
        return pltpu.make_async_remote_copy(
            src_ref=piece,
            dst_ref=piece,
            send_sem=w_send.at[kind * n + d],
            recv_sem=w_recv.at[kind * n + d],
            device_id=(sp, across if kind == 0 else beside),
            device_id_type=MESH,
        )

    def pass_on(d):
        if d == 0:
            own_piece.wait()
        else:
            slot = lax.rem(sp - d + n, n)
            piece = wall.at[slot, :, units(tp), :]
            pltpu.make_async_remote_copy(
                src_ref=piece,
                dst_ref=piece,
                send_sem=a_send.at[d - 1],
                recv_sem=a_recv.at[d - 1],
                device_id=(lax.rem(sp + d, n), tp),
                device_id_type=MESH,
            ).wait_recv()
        for kind in (0, 1):
            copy = relay(kind, d)
            copy.start()
            started.append(copy)

    spread(1)
    spread(2)
    pass_on(0)

    for h in range(groups):
        qs[h] = turned(q_in[:, h * hd : (h + 1) * hd], qg_ref[...])
    m_s[...] = jnp.full_like(m_s, -1e30)
    l_s[...] = jnp.zeros_like(l_s)
    acc[...] = jnp.zeros_like(acc)
    factor = hd ** (-0.5) * math.log2(math.e)

    def attend(slots):
        def one(i, carry):
            h = lax.rem(i, groups)
            slot = slots[0]
            if len(slots) > 1:
                slot = jnp.where(i < groups, slots[0], slots[1])
            scores = lax.dot_general(
                qs[h], kbuf[slot], (((1,), (1,)), ((), ())), preferred_element_type=jnp.float32
            )
            before = m_s[h]
            highest = jnp.maximum(before, jnp.max(scores, axis=-1, keepdims=True))
            scale = jnp.exp2((before - highest) * factor)
            probs = jnp.exp2((scores - highest) * factor)
            m_s[h] = highest
            l_s[h] = l_s[h] * scale + jnp.sum(probs, axis=-1, keepdims=True)
            acc[h] = acc[h] * scale + jnp.dot(
                probs.astype(jnp.bfloat16), vbuf[slot], preferred_element_type=jnp.float32
            )
            return carry

        lax.fori_loop(0, groups * len(slots), one, 0)

    attend([sp])
    for step in range(1, half + 1):
        arrive("k", step)
        arrive("v", step)
        for d in (2 * step + 1, 2 * step + 2):
            if d < n:
                spread(d)
        ends = [ring_at(pos - step), ring_at(pos + step)]
        attend(ends if step < half else ends[:1])
        for d in (2 * step - 5, 2 * step - 4):
            if 0 < d < n:
                pass_on(d)

    for h in range(groups):
        done = (acc[h] / l_s[h]).astype(jnp.bfloat16)
        for t in range(tn):
            att[t, :, h * hd : (h + 1) * hd] = done[t * rows : (t + 1) * rows]
    to_heads = []
    for d in range(1, tn):
        peer = lax.rem(tp + d, tn)
        copy = pltpu.make_async_remote_copy(
            src_ref=att.at[peer],
            dst_ref=heads.at[tp],
            send_sem=tp_send.at[d - 1],
            recv_sem=tp_recv.at[d - 1],
            device_id=(sp, peer),
            device_id_type=MESH,
        )
        copy.start()
        to_heads.append(copy)
    heads[tp] = att[tp]
    for d in range(2 * half - 3, n):
        pass_on(d)
    locs["o"].wait()
    for copy in to_heads:
        copy.wait_recv()

    span = math.gcd(ow.shape[1], 512)

    def project(i, carry):
        cols = pl.ds(pl.multiple_of(i * span, span), span)
        total = jnp.zeros((rows, span), jnp.float32)
        for t in range(tn):
            total += jnp.dot(
                heads[t], ow[t * width : (t + 1) * width, cols], preferred_element_type=jnp.float32
            )
        proj[:, cols] = total
        return carry

    lax.fori_loop(0, ow.shape[1] // span, project, 0)
    projected = proj[...]
    middle = (
        res_ref[...].astype(jnp.float32)
        + og_ref[...]
        * (projected * lax.rsqrt(jnp.mean(projected * projected, axis=-1, keepdims=True) + EPS))
    ).astype(jnp.bfloat16)
    mid[...] = middle
    middle = middle.astype(jnp.float32)
    normed = (
        mg_ref[...] * (middle * lax.rsqrt(jnp.mean(middle * middle, axis=-1, keepdims=True) + EPS))
    ).astype(jnp.bfloat16)

    for way in range(2):
        toks[way, sp] = normed[way * side : (way + 1) * side]

    def token_copy(way, step):
        origin = ring_at(pos - (step - 1)) if way == 0 else ring_at(pos + (step - 1))
        return pltpu.make_async_remote_copy(
            src_ref=toks.at[way, origin],
            dst_ref=toks.at[way, origin],
            send_sem=t_send.at[way * n + step],
            recv_sem=t_recv.at[way * n + step],
            device_id=(right if way == 0 else left, tp),
            device_id_type=MESH,
        )

    def sum_copy(way, step):
        return pltpu.make_async_remote_copy(
            src_ref=psend.at[way, step],
            dst_ref=precv.at[way, step],
            send_sem=p_send.at[way * n + step],
            recv_sem=p_recv.at[way * n + step],
            device_id=(right if way == 0 else left, tp),
            device_id_type=MESH,
        )

    for way in range(2):
        token_copy(way, 1).start()
    for d in range(n):
        relay(0, d).wait_recv()
        copy = relay(2, d)
        copy.start()
        started.append(copy)
    for d in range(n):
        relay(1, d).wait_recv()
        relay(2, d).wait_recv()

    def block(step, carry):
        for way in range(2):

            @pl.when(step > 0)
            def _():
                token_copy(way, step).wait_recv()

            @pl.when(jnp.logical_and(step > 0, step < n - 1))
            def _():
                token_copy(way, step + 1).start()

        tokens = jnp.concatenate(
            [toks[0, ring_at(pos - step)], toks[1, ring_at(pos + step)]], axis=0
        )
        branches = []
        for which in range(2):
            total = jnp.zeros((rows, hidden // n * tn), jnp.float32)
            for s in range(n):
                total += lax.dot_general(
                    tokens[:, s * depth : (s + 1) * depth],
                    wall[s, which],
                    (((1,), (1,)), ((), ())),
                    preferred_element_type=jnp.float32,
                )
            branches.append(total)
        gate, up = branches
        inner = (gate / (1.0 + jnp.exp(-gate)) * up).astype(jnp.bfloat16)
        for s in range(n):
            osc[:, s * depth : (s + 1) * depth] = jnp.dot(
                inner, wall[s, 2], preferred_element_type=jnp.float32
            )

        @pl.when(step == 0)
        def _():
            proj[...] = osc[...]

        @pl.when(step > 0)
        def _():
            for way in range(2):
                part = slice(way * side, (way + 1) * side)

                @pl.when(step > 1)
                def _():
                    sum_copy(way, step - 1).wait_recv()
                    osc[part] += precv[way, step - 1].astype(jnp.float32)

                psend[way, step] = osc[part].astype(jnp.bfloat16)
                sum_copy(way, step).start()

        return carry

    lax.fori_loop(0, n, block, 0)
    for way in range(2):
        sum_copy(way, n - 1).wait_recv()
        part = slice(way * side, (way + 1) * side)
        proj[part] += precv[way, n - 1].astype(jnp.float32)
    total = proj[...]
    out_ref[...] = (
        mid[...].astype(jnp.float32)
        + fg_ref[...] * (total * lax.rsqrt(jnp.mean(total * total, axis=-1, keepdims=True) + EPS))
    ).astype(jnp.bfloat16)
    for copy in started + to_heads:
        copy.wait_send()

    def drain(step, carry):
        for way in range(2):
            token_copy(way, step).wait_send()
            sum_copy(way, step).wait_send()
        return carry

    lax.fori_loop(1, n, drain, 0)


def rotary_tables(tok_rows, head_size):
    quarter = head_size // 4
    positions = lax.axis_index("sp") * tok_rows + jnp.arange(tok_rows, dtype=jnp.int32)
    lane = jnp.arange(head_size, dtype=jnp.int32)
    freqs = 10000.0 ** (-(lane % quarter).astype(jnp.float32) / quarter)
    row = (positions // GRID_W).astype(jnp.float32)[:, None]
    column = (positions % GRID_W).astype(jnp.float32)[:, None]
    angle = jnp.where(lane < 2 * quarter, row, column) * freqs
    sine = jnp.sin(angle)
    return jnp.cos(angle), jnp.where(lane % (2 * quarter) < quarter, -sine, sine)


def fused(n, tn, *args):
    (queries, keys, values, q_gain, k_gain, out_weight, out_gain, residual_in) = args[:8]
    (mlp_gain, gate_weight, up_weight, down_weight, final_gain) = args[8:]
    tok, hd = keys.shape
    groups = queries.shape[1] // hd
    depth, hidden = gate_weight.shape
    rows, wide = residual_in.shape
    cosine, sine = rotary_tables(tok, hd)
    vmem = pl.BlockSpec(memory_space=pltpu.VMEM)
    hbm = pl.BlockSpec(memory_space=pl.ANY)
    half = n // 2
    b16, f32 = jnp.bfloat16, jnp.float32
    return pl.pallas_call(
        functools.partial(layer_kernel, n, tn),
        out_shape=jax.ShapeDtypeStruct((rows, wide), b16),
        in_specs=[vmem, vmem, hbm, vmem, vmem, vmem, vmem, hbm, vmem, vmem, vmem, hbm, hbm, hbm, vmem],
        out_specs=vmem,
        scratch_shapes=[
            pltpu.VMEM((groups, tok, hd), b16),
            pltpu.VMEM((n, tok, hd), b16),
            pltpu.VMEM((n, tok, hd), b16),
            pltpu.VMEM((2, depth, hidden), b16),
            pltpu.VMEM((3, hidden, depth), b16),
            pltpu.VMEM((n, 3, hidden // n * tn, depth), b16),
            pltpu.VMEM((wide, wide), b16),
            pltpu.VMEM((groups, tok, 1), f32),
            pltpu.VMEM((groups, tok, 1), f32),
            pltpu.VMEM((groups, tok, hd), f32),
            pltpu.VMEM((tn, rows, groups * hd), b16),
            pltpu.VMEM((tn, rows, groups * hd), b16),
            pltpu.VMEM((rows, wide), f32),
            pltpu.VMEM((rows, wide), b16),
            pltpu.VMEM((2, n, rows // 2, wide), b16),
            pltpu.VMEM((rows, wide), f32),
            pltpu.VMEM((2, n, rows // 2, wide), b16),
            pltpu.VMEM((2, n, rows // 2, wide), b16),
            pltpu.SemaphoreType.DMA((6,)),
            pltpu.SemaphoreType.DMA((4 * half,)),
            pltpu.SemaphoreType.DMA((4 * half,)),
            pltpu.SemaphoreType.DMA((tn - 1,)),
            pltpu.SemaphoreType.DMA((tn - 1,)),
            pltpu.SemaphoreType.DMA((n - 1,)),
            pltpu.SemaphoreType.DMA((n - 1,)),
            pltpu.SemaphoreType.DMA((3 * n,)),
            pltpu.SemaphoreType.DMA((3 * n,)),
            pltpu.SemaphoreType.DMA((2 * n,)),
            pltpu.SemaphoreType.DMA((2 * n,)),
            pltpu.SemaphoreType.DMA((2 * n,)),
            pltpu.SemaphoreType.DMA((2 * n,)),
        ],
        compiler_params=pltpu.CompilerParams(
            collective_id=0, has_side_effects=True, vmem_limit_bytes=67043328
        ),
    )(
        queries,
        keys,
        values,
        cosine,
        sine,
        q_gain[None],
        k_gain[None],
        out_weight,
        out_gain[None],
        residual_in,
        mlp_gain[None],
        gate_weight,
        up_weight,
        down_weight,
        final_gain[None],
    )


def body(mesh, *args):
    n, tn = mesh.shape["sp"], mesh.shape["tp"]
    tok, hd = args[1].shape
    depth, hidden = args[9].shape
    fits = n % 2 == 0 and 4 <= n <= 8 and depth % 128 == 0 and hidden % 128 == 0
    fits = fits and tn == 4 and hidden % (16 * n) == 0 and args[7].shape[0] % 32 == 0
    if fits and tok % 256 == 0 and hd == 128:
        return fused(n, tn, *args)
    return on_device(*args)


def solution(mesh):
    return jax.shard_map(
        functools.partial(body, mesh),
        mesh=mesh,
        in_specs=(
            P("sp", "tp"),
            P("sp", "tp"),
            P("sp", "tp"),
            P(),
            P(),
            P(),
            P(),
            P(("sp", "tp"), None),
            P(),
            P("sp", "tp"),
            P("sp", "tp"),
            P("tp", "sp"),
            P(),
        ),
        out_specs=P(("sp", "tp"), None),
        check_vma=False,
    )
```

```python
import functools
import math

import jax
import jax.numpy as jnp
from jax import lax
from jax.experimental import pallas as pl
from jax.experimental.pallas import tpu as pltpu
from jax.sharding import PartitionSpec as P

GRID_W = 64


def rms_scale(matrix):
    return matrix * lax.rsqrt(jnp.mean(matrix * matrix, axis=-1, keepdims=True) + 1e-06)


def rotary(matrix, positions):
    quarter = matrix.shape[-1] // 4
    freqs = 10000.0 ** (-jnp.arange(quarter, dtype=jnp.float32) / quarter)
    grid = jnp.stack([positions // GRID_W, positions % GRID_W], axis=-1).astype(jnp.float32)
    angle = grid[:, :, None] * freqs
    cosine = jnp.cos(angle)[:, None]
    sine = jnp.sin(angle)[:, None]
    parts = matrix.reshape(matrix.shape[:-1] + (2, 2, quarter))
    first = parts[..., 0, :]
    second = parts[..., 1, :]
    turned = jnp.stack([first * cosine - second * sine, second * cosine + first * sine], axis=-2)
    return turned.reshape(matrix.shape)


def on_device(
    queries,
    keys,
    values,
    q_gain,
    k_gain,
    out_weight,
    out_gain,
    residual_in,
    mlp_gain,
    gate_weight,
    up_weight,
    down_weight,
    final_gain,
):
    tok_rows = queries.shape[0]
    head_size = q_gain.shape[0]
    q_heads = queries.shape[1] // head_size
    kv_heads = keys.shape[1] // head_size
    group_size = q_heads // kv_heads
    positions = lax.axis_index("sp") * tok_rows + jnp.arange(tok_rows, dtype=jnp.int32)
    query_rot = rotary(
        rms_scale(queries.reshape(tok_rows, q_heads, head_size).astype(jnp.float32)) * q_gain,
        positions,
    ).astype(jnp.bfloat16)
    key_rot = rotary(
        rms_scale(keys.reshape(tok_rows, kv_heads, head_size).astype(jnp.float32)) * k_gain,
        positions,
    ).astype(jnp.bfloat16)
    key_flat = key_rot.reshape(tok_rows, kv_heads * head_size)
    grouped = query_rot.reshape(tok_rows, kv_heads, group_size, head_size)
    score_scale = head_size ** (-0.5)
    key_all, value_all = (
        lax.all_gather(key_flat, "sp", axis=0, tiled=True),
        lax.all_gather(values, "sp", axis=0, tiled=True),
    )
    total_rows = key_all.shape[0]
    span = math.gcd(total_rows, 1024)
    key_blocks = key_all.reshape(total_rows // span, span, kv_heads, head_size)
    value_blocks = value_all.reshape(total_rows // span, span, kv_heads, head_size)

    def step(run_state, blocks):
        highest, weight_sum, accum = run_state
        key_block, value_block = blocks
        scores = (
            jnp.einsum("qcgd,kcd->cgqk", grouped, key_block, preferred_element_type=jnp.float32)
            * score_scale
        )
        new_high = jnp.maximum(highest, jnp.max(scores, axis=-1))
        factor = jnp.exp(highest - new_high)
        exp_scores = jnp.exp(scores - new_high[..., None])
        weight_sum = weight_sum * factor + jnp.sum(exp_scores, axis=-1)
        accum = accum * factor[..., None] + jnp.einsum(
            "cgqk,kcd->cgqd",
            exp_scores.astype(jnp.bfloat16),
            value_block,
            preferred_element_type=jnp.float32,
        )
        return ((new_high, weight_sum, accum), None)

    start_state = (
        jnp.full((kv_heads, group_size, tok_rows), -1e30, jnp.float32),
        jnp.zeros((kv_heads, group_size, tok_rows), jnp.float32),
        jnp.zeros((kv_heads, group_size, tok_rows, head_size), jnp.float32),
    )
    final_state, unused = lax.scan(step, start_state, (key_blocks, value_blocks))
    highest, weight_sum, accum = final_state
    attended = (
        jnp.transpose(accum / weight_sum[..., None], (2, 0, 1, 3))
        .reshape(tok_rows, q_heads * head_size)
        .astype(jnp.bfloat16)
    )
    head_rows = lax.all_to_all(attended, "tp", split_axis=0, concat_axis=1, tiled=True)
    projected = jnp.dot(head_rows, out_weight, preferred_element_type=jnp.float32)
    mid_stream = (residual_in.astype(jnp.float32) + out_gain * rms_scale(projected)).astype(
        jnp.bfloat16
    )
    normed = (mlp_gain * rms_scale(mid_stream.astype(jnp.float32))).astype(jnp.bfloat16)
    mixer_in = lax.all_gather(normed, "tp", axis=0, tiled=True)
    gate_proj = jnp.dot(
        mixer_in,
        lax.all_gather(gate_weight, "sp", axis=0, tiled=True),
        preferred_element_type=jnp.float32,
    )
    up_proj = jnp.dot(
        mixer_in,
        lax.all_gather(up_weight, "sp", axis=0, tiled=True),
        preferred_element_type=jnp.float32,
    )
    down_full = lax.all_gather(down_weight, "sp", axis=1, tiled=True)
    hidden = (jax.nn.silu(gate_proj) * up_proj).astype(jnp.bfloat16)
    mlp_branch = lax.psum_scatter(
        jnp.dot(hidden, down_full, preferred_element_type=jnp.float32).astype(jnp.bfloat16),
        "tp",
        scatter_dimension=0,
        tiled=True,
    ).astype(jnp.float32)
    return (mid_stream.astype(jnp.float32) + final_gain * rms_scale(mlp_branch)).astype(
        jnp.bfloat16
    )


MESH = pl.DeviceIdType.MESH
EPS = 1e-06


def layer_kernel(
    n,
    tn,
    q_in,
    k_in,
    v_hbm,
    qg_ref,
    kg_ref,
    ow_hbm,
    og_ref,
    res_ref,
    mg_ref,
    gate_hbm,
    up_hbm,
    down_hbm,
    fg_ref,
    out_ref,
    cos_ref,
    sin_ref,
    qs,
    kbuf,
    vbuf,
    gbuf,
    ubuf,
    dbuf,
    ow,
    m_s,
    l_s,
    acc,
    att,
    heads,
    proj,
    mid,
    mix,
    gacc,
    uacc,
    hid,
    pbuf,
    rbuf,
    loc_sem,
    send_sem,
    recv_sem,
    tp_send,
    tp_recv,
    pt_send,
    pt_recv,
):
    sp = lax.axis_index("sp")
    tp = lax.axis_index("tp")
    half = n // 2

    def ring_at(pos):
        pos = lax.rem(pos + 2 * n, n)
        return jnp.where(pos < half, 2 * pos, 2 * (n - 1 - pos) + 1)

    pos = jnp.where(lax.rem(sp, 2) == 0, sp // 2, n - 1 - sp // 2)
    right, left = ring_at(pos + 1), ring_at(pos - 1)
    tok, hd = k_in.shape
    groups = q_in.shape[1] // hd
    depth = gate_hbm.shape[0]
    hidden = gate_hbm.shape[1]
    rows = res_ref.shape[0]
    width = groups * hd

    locs = {
        "v": pltpu.make_async_copy(v_hbm, vbuf.at[sp], loc_sem.at[0]),
        "g": pltpu.make_async_copy(gate_hbm, gbuf.at[sp], loc_sem.at[1]),
        "u": pltpu.make_async_copy(up_hbm, ubuf.at[sp], loc_sem.at[2]),
        "d": pltpu.make_async_copy(down_hbm, dbuf.at[sp], loc_sem.at[3]),
        "o": pltpu.make_async_copy(ow_hbm, ow, loc_sem.at[4]),
    }
    for name in "vgudo":
        locs[name].start()

    lane = lax.broadcasted_iota(jnp.int32, (tok, hd), 1)
    quarter = hd // 4
    first = lax.rem(lane, 2 * quarter) < quarter

    def turned(x, gain):
        x = x.astype(jnp.float32)
        x = x * lax.rsqrt(jnp.mean(x * x, axis=-1, keepdims=True) + EPS) * gain
        other = jnp.where(first, pltpu.roll(x, hd - quarter, 1), pltpu.roll(x, quarter, 1))
        return (x * cos_ref[...] + other * sin_ref[...]).astype(jnp.bfloat16)

    barrier = pltpu.get_barrier_semaphore()
    for peer in (left, right):
        pl.semaphore_signal(barrier, inc=1, device_id=(peer, tp), device_id_type=MESH)
    for d in range(1, tn):
        pl.semaphore_signal(
            barrier, inc=1, device_id=(sp, lax.rem(tp + d, tn)), device_id_type=MESH
        )
    pl.semaphore_wait(barrier, 2 + tn - 1)

    cut = hidden // 2
    items = {
        "k": (0, half, lambda s: kbuf.at[s]),
        "v": (1, half - 1, lambda s: vbuf.at[s]),
        "g": (2, half, lambda s: gbuf.at[s]),
        "u": (3, half - 1, lambda s: ubuf.at[s]),
        "a": (4, half, lambda s: dbuf.at[s, pl.ds(0, cut), :]),
        "b": (5, half - 1, lambda s: dbuf.at[s, pl.ds(cut, hidden - cut), :]),
    }
    started = []

    def copies(name, step):
        number, to_right, view = items[name]
        found = []
        for way, count in ((0, to_right), (1, n - 1 - to_right)):
            if step > count:
                continue
            origin = ring_at(pos - (step - 1)) if way == 0 else ring_at(pos + (step - 1))
            index = (number * 2 + way) * half + step - 1
            found.append(
                pltpu.make_async_remote_copy(
                    src_ref=view(origin),
                    dst_ref=view(origin),
                    send_sem=send_sem.at[index],
                    recv_sem=recv_sem.at[index],
                    device_id=(right if way == 0 else left, tp),
                    device_id_type=MESH,
                )
            )
        return found

    def send(name, step):
        for copy in copies(name, step):
            copy.start()
            started.append(copy)

    def arrive(name, step, then=True):
        number, to_right, view = items[name]
        for way, count in ((0, to_right), (1, n - 1 - to_right)):
            if step > count:
                continue
            origin = ring_at(pos - step) if way == 0 else ring_at(pos + step)
            index = (number * 2 + way) * half + step - 1
            pltpu.make_async_remote_copy(
                src_ref=view(origin),
                dst_ref=view(origin),
                send_sem=send_sem.at[index],
                recv_sem=recv_sem.at[index],
                device_id=(right if way == 0 else left, tp),
                device_id_type=MESH,
            ).wait_recv()
            if step < count:
                index += 1
                copy = pltpu.make_async_remote_copy(
                    src_ref=view(origin),
                    dst_ref=view(origin),
                    send_sem=send_sem.at[index],
                    recv_sem=recv_sem.at[index],
                    device_id=(right if way == 0 else left, tp),
                    device_id_type=MESH,
                )
                copy.start()
                started.append(copy)

    for name in "gu":
        locs[name].wait()
        send(name, 1)

    place = sp * tok + lax.broadcasted_iota(jnp.int32, (tok, hd), 0)
    place = jnp.where(lane < 2 * quarter, place // GRID_W, lax.rem(place, GRID_W))
    turn = lax.rem(lane, quarter).astype(jnp.float32)
    angle = place.astype(jnp.float32) * jnp.exp(turn * (-math.log(10000.0) / quarter))
    cos_ref[...] = jnp.cos(angle)
    sine = jnp.sin(angle)
    sin_ref[...] = jnp.where(first, -sine, sine)
    kbuf[sp] = turned(k_in[...], kg_ref[...])
    locs["v"].wait()
    send("v", 1)
    send("k", 1)

    for h in range(groups):
        qs[h] = turned(q_in[:, h * hd : (h + 1) * hd], qg_ref[...])
    m_s[...] = jnp.full_like(m_s, -1e30)
    l_s[...] = jnp.zeros_like(l_s)
    acc[...] = jnp.zeros_like(acc)
    factor = hd ** (-0.5) * math.log2(math.e)

    def attend(slots):
        def one(i, carry):
            h = lax.rem(i, groups)
            slot = slots[0]
            if len(slots) > 1:
                slot = jnp.where(i < groups, slots[0], slots[1])
            scores = lax.dot_general(
                qs[h], kbuf[slot], (((1,), (1,)), ((), ())), preferred_element_type=jnp.float32
            )
            before = m_s[h]
            highest = jnp.maximum(before, jnp.max(scores, axis=-1, keepdims=True))
            scale = jnp.exp2((before - highest) * factor)
            probs = jnp.exp2((scores - highest) * factor)
            m_s[h] = highest
            l_s[h] = l_s[h] * scale + jnp.sum(probs, axis=-1, keepdims=True)
            acc[h] = acc[h] * scale + jnp.dot(
                probs.astype(jnp.bfloat16), vbuf[slot], preferred_element_type=jnp.float32
            )
            return carry

        lax.fori_loop(0, groups * len(slots), one, 0)

    attend([sp])
    for step in range(1, half + 1):
        arrive("ug"[step % 2], (step + 1) // 2)
        arrive("k", step)
        arrive("v", step)
        if step == 1:
            locs["d"].wait()
        ends = [ring_at(pos - step), ring_at(pos + step)]
        attend(ends if step < half else ends[:1])

    for h in range(groups):
        done = (acc[h] / l_s[h]).astype(jnp.bfloat16)
        for t in range(tn):
            att[t, :, h * hd : (h + 1) * hd] = done[t * rows : (t + 1) * rows]
    to_heads = []
    for d in range(1, tn):
        peer = lax.rem(tp + d, tn)
        copy = pltpu.make_async_remote_copy(
            src_ref=att.at[peer],
            dst_ref=heads.at[tp],
            send_sem=tp_send.at[d - 1],
            recv_sem=tp_recv.at[d - 1],
            device_id=(sp, peer),
            device_id_type=MESH,
        )
        copy.start()
        to_heads.append(copy)
    heads[tp] = att[tp]
    late = [(name, step) for step in range(1, half + 1) for name in "gu"]
    seen = [("ug"[s % 2], (s + 1) // 2) for s in range(1, half + 1)]
    late = [event for event in late if event not in seen]
    locs["o"].wait()
    for copy in to_heads:
        copy.wait_recv()

    span = math.gcd(ow.shape[1], 512)

    def project(i, carry):
        cols = pl.ds(pl.multiple_of(i * span, span), span)
        total = jnp.zeros((rows, span), jnp.float32)
        for t in range(tn):
            total += jnp.dot(
                heads[t], ow[t * width : (t + 1) * width, cols], preferred_element_type=jnp.float32
            )
        proj[:, cols] = total
        return carry

    lax.fori_loop(0, ow.shape[1] // span, project, 0)
    projected = proj[...]
    middle = (
        res_ref[...].astype(jnp.float32)
        + og_ref[...]
        * (projected * lax.rsqrt(jnp.mean(projected * projected, axis=-1, keepdims=True) + EPS))
    ).astype(jnp.bfloat16)
    mid[...] = middle
    middle = middle.astype(jnp.float32)
    normed = (
        mg_ref[...] * (middle * lax.rsqrt(jnp.mean(middle * middle, axis=-1, keepdims=True) + EPS))
    ).astype(jnp.bfloat16)
    mine = pl.ds(pl.multiple_of(tp * rows, rows), rows)
    for s in range(n):
        mix[s, mine, :] = normed[:, s * depth : (s + 1) * depth]
    to_mix = []
    for d in range(1, tn):
        peer = lax.rem(tp + d, tn)
        copy = pltpu.make_async_remote_copy(
            src_ref=mix.at[:, mine, :],
            dst_ref=mix.at[:, mine, :],
            send_sem=tp_send.at[tn - 1 + d - 1],
            recv_sem=tp_recv.at[tn - 1 + d - 1],
            device_id=(sp, peer),
            device_id_type=MESH,
        )
        copy.start()
        to_mix.append(copy)

    for event in late[: len(late) // 2]:
        arrive(*event)
    send("a", 1)
    send("b", 1)
    gacc[...] = jnp.zeros_like(gacc)
    uacc[...] = jnp.zeros_like(uacc)
    for copy in to_mix:
        copy.wait_recv()
    tile = math.gcd(tok, 256)

    def add_block(buf, total, slot):
        def one(i, carry):
            part = pl.ds(pl.multiple_of(i * tile, tile), tile)
            total[part, :] += jnp.dot(
                mix[slot, part, :], buf[slot], preferred_element_type=jnp.float32
            )
            return carry

        lax.fori_loop(0, tok // tile, one, 0)

    def add_blocks(name, slots):
        buf, total = (gbuf, gacc) if name == "g" else (ubuf, uacc)
        slots = list(slots)

        def one(i, carry):
            slot = slots[0]
            for place, other in enumerate(slots[1:]):
                slot = jnp.where(i > place, other, slot)
            add_block(buf, total, slot)
            return carry

        lax.fori_loop(0, len(slots), one, 0)

    def origins(name, step):
        to_right = items[name][1]
        found = []
        if step <= to_right:
            found.append(ring_at(pos - step))
        if step <= n - 1 - to_right:
            found.append(ring_at(pos + step))
        return found

    ready = {"g": [sp], "u": [sp]}
    for name, step in seen + late[: len(late) // 2]:
        ready[name] += origins(name, step)
    for name in "gu":
        add_blocks(name, ready[name])
    for name, step in late[len(late) // 2 :]:
        arrive(name, step)
        add_blocks(name, origins(name, step))

    def activate(i, carry):
        part = pl.ds(pl.multiple_of(i * 64, 64), 64)
        gate = gacc[part, :]
        hid[part, :] = (gate / (1.0 + jnp.exp(-gate)) * uacc[part, :]).astype(jnp.bfloat16)
        return carry

    lax.fori_loop(0, tok // 64, activate, 0)

    def shares(number, slot):
        def one(t, carry):
            part = pl.ds(pl.multiple_of(t * rows, rows), rows)
            pbuf[slot, t] = jnp.dot(
                hid[part, :], dbuf[slot], preferred_element_type=jnp.float32
            ).astype(jnp.bfloat16)
            return carry

        lax.fori_loop(0, tn, one, 0)
        for d in range(1, tn):
            peer = lax.rem(tp + d, tn)
            index = number * (tn - 1) + d - 1
            copy = pltpu.make_async_remote_copy(
                src_ref=pbuf.at[slot, peer],
                dst_ref=rbuf.at[tp, slot],
                send_sem=pt_send.at[index],
                recv_sem=pt_recv.at[index],
                device_id=(sp, peer),
                device_id_type=MESH,
            )
            copy.start()
            last.append(copy)
        rbuf[tp, slot] = pbuf[slot, tp]

    last = []
    shares(0, sp)
    number = 1
    for step in range(1, half + 1):
        arrive("a", step)
        arrive("b", step)
        if step < half:
            for slot in (ring_at(pos - step), ring_at(pos + step)):
                shares(number, slot)
                number += 1
        else:
            shares(number, ring_at(pos - step))
    for copy in last:
        copy.wait_recv()
    square = jnp.zeros((rows, 1), jnp.float32)
    for s in range(n):
        total = rbuf[0, s].astype(jnp.float32)
        for t in range(1, tn):
            total += rbuf[t, s].astype(jnp.float32)
        proj[:, s * depth : (s + 1) * depth] = total
        square += jnp.sum(total * total, axis=-1, keepdims=True)
    scale = lax.rsqrt(square / (n * depth) + EPS)
    out_ref[...] = (mid[...].astype(jnp.float32) + fg_ref[...] * (proj[...] * scale)).astype(
        jnp.bfloat16
    )
    for copy in started + to_heads + to_mix + last:
        copy.wait_send()


def fused(n, tn, *args):
    (queries, keys, values, q_gain, k_gain, out_weight, out_gain, residual_in) = args[:8]
    (mlp_gain, gate_weight, up_weight, down_weight, final_gain) = args[8:]
    tok, hd = keys.shape
    groups = queries.shape[1] // hd
    depth, hidden = gate_weight.shape
    rows, wide = residual_in.shape
    vmem = pl.BlockSpec(memory_space=pltpu.VMEM)
    hbm = pl.BlockSpec(memory_space=pl.ANY)
    half = n // 2
    b16, f32 = jnp.bfloat16, jnp.float32
    return pl.pallas_call(
        functools.partial(layer_kernel, n, tn),
        out_shape=jax.ShapeDtypeStruct((rows, wide), b16),
        in_specs=[vmem, vmem, hbm, vmem, vmem, hbm, vmem, vmem, vmem, hbm, hbm, hbm, vmem],
        out_specs=vmem,
        scratch_shapes=[
            pltpu.VMEM((tok, hd), f32),
            pltpu.VMEM((tok, hd), f32),
            pltpu.VMEM((groups, tok, hd), b16),
            pltpu.VMEM((n, tok, hd), b16),
            pltpu.VMEM((n, tok, hd), b16),
            pltpu.VMEM((n, depth, hidden), b16),
            pltpu.VMEM((n, depth, hidden), b16),
            pltpu.VMEM((n, hidden, depth), b16),
            pltpu.VMEM((wide, wide), b16),
            pltpu.VMEM((groups, tok, 1), f32),
            pltpu.VMEM((groups, tok, 1), f32),
            pltpu.VMEM((groups, tok, hd), f32),
            pltpu.VMEM((tn, rows, groups * hd), b16),
            pltpu.VMEM((tn, rows, groups * hd), b16),
            pltpu.VMEM((rows, wide), f32),
            pltpu.VMEM((rows, wide), b16),
            pltpu.VMEM((n, tok, depth), b16),
            pltpu.VMEM((tok, hidden), f32),
            pltpu.VMEM((tok, hidden), f32),
            pltpu.VMEM((tok, hidden), b16),
            pltpu.VMEM((n, tn, rows, depth), b16),
            pltpu.VMEM((tn, n, rows, depth), b16),
            pltpu.SemaphoreType.DMA((5,)),
            pltpu.SemaphoreType.DMA((12 * half,)),
            pltpu.SemaphoreType.DMA((12 * half,)),
            pltpu.SemaphoreType.DMA((2 * (tn - 1),)),
            pltpu.SemaphoreType.DMA((2 * (tn - 1),)),
            pltpu.SemaphoreType.DMA((n * (tn - 1),)),
            pltpu.SemaphoreType.DMA((n * (tn - 1),)),
        ],
        compiler_params=pltpu.CompilerParams(
            collective_id=0, has_side_effects=True, vmem_limit_bytes=67043328
        ),
    )(
        queries,
        keys,
        values,
        q_gain[None],
        k_gain[None],
        out_weight,
        out_gain[None],
        residual_in,
        mlp_gain[None],
        gate_weight,
        up_weight,
        down_weight,
        final_gain[None],
    )


def body(mesh, *args):
    n, tn = mesh.shape["sp"], mesh.shape["tp"]
    tok, hd = args[1].shape
    depth, hidden = args[9].shape
    fits = n % 2 == 0 and 4 <= n <= 8 and depth % 128 == 0 and hidden % 32 == 0
    if fits and tok % 256 == 0 and hd == 128:
        return fused(n, tn, *args)
    return on_device(*args)


def solution(mesh):
    return jax.shard_map(
        functools.partial(body, mesh),
        mesh=mesh,
        in_specs=(
            P("sp", "tp"),
            P("sp", "tp"),
            P("sp", "tp"),
            P(),
            P(),
            P(),
            P(),
            P(("sp", "tp"), None),
            P(),
            P("sp", "tp"),
            P("sp", "tp"),
            P("tp", "sp"),
            P(),
        ),
        out_specs=P(("sp", "tp"), None),
        check_vma=False,
    )
```
